128 devices in a mesh: ep: 32 (over z, y, core), tp: 4 (over x).
Axes of the slice: x: 4, y: 4, z: 4, core: 2. Of those that a mesh axis runs over, the one named last changes fastest.
Arguments:
- query_rows: bfloat16 [16384, 1024], P('ep', 'tp'), may hold values from -10 to 10
- key_rows: bfloat16 [16384, 1024], P('ep', 'tp'), may hold values from -10 to 10
- value_rows: bfloat16 [16384, 1024], P('ep', 'tp'), may hold values from -6 to 6
- key_bias: float32 [16384, 16], P(None, 'tp'), may hold values from -30 to 0
- out_weight: bfloat16 [1024, 2048], P('tp'), may hold values from -0.5625 to 0.5625
- moe_input: bfloat16 [16384, 2048], P(('ep', 'tp')), may hold values from -6 to 6
- moe_gain: float32 [2048], replicated, may hold values from 0.1 to 1.9
- expert_pick: int32 [16384, 2], P(('ep', 'tp')), may hold values from 0 to 31, as said below
- route_weight: float32 [16384, 2], P(('ep', 'tp')), may hold values from 0.1 to 1
- w_gate: bfloat16 [32, 2048, 1024], P('ep', None, 'tp'), may hold values from -0.125 to 0.125
- w_up: bfloat16 [32, 2048, 1024], P('ep', None, 'tp'), may hold values from -0.125 to 0.125
- w_down: bfloat16 [32, 1024, 2048], P('ep', 'tp'), may hold values from -0.1875 to 0.1875
Outputs:
- mixer_out: bfloat16 [16384, 2048], P(('ep', 'tp'))
- routed_out: bfloat16 [16384, 2048], P(('ep', 'tp'))
The draws below stay inside these ranges and needn't reach their ends.
Inputs may be any that keep to these rules, and one draw needn't show every extreme that they name: `expert_pick`: each row names two different experts of one group, expert e belonging to group e // 8; the rows of one device name no expert more than 16 times, and in every draw each expert of some group is named exactly 16 times by the rows of every device.
All inputs are finite; a program needn't handle non-finite values.
Results may differ from the reference program's by a relative error of at most 0.013.
Values may be sent and summed in bfloat16 or wider, within the bound.
A program may use at most 128 MiB of HBM per device.

```python
import math
import jax
import jax.numpy as jnp
from jax import lax

D = 2048
ATTENTION_HEADS = 16
HEAD_DIM = 64
FF = 1024
GROUPS = 4
TOPK = 2
SEQ_DEV = 512
TOK2_DEV = 128
EXPERTS = 32
FIRST_TOKENS1 = 16384
SEQ_BLOCKS = 32
TOKENS2 = 16384
CAP = 16
N_TP = 4


def draw_key_bias(key, part):
    flow_lanes = jax.random.split(jax.random.fold_in(key, 101), 5)
    fast_heads = jax.random.uniform(flow_lanes[0], (ATTENTION_HEADS,)) < 0.5
    jitter = jnp.clip(0.5 * jax.random.normal(flow_lanes[2], (FIRST_TOKENS1, ATTENTION_HEADS)), -1.0, 1.0)
    base_level = jnp.where(fast_heads, -jnp.log(4000.0), -jnp.log(130.0 * FIRST_TOKENS1))
    block_count = FIRST_TOKENS1 // SEQ_DEV
    shifts = jax.random.uniform(flow_lanes[1], (block_count, 1, ATTENTION_HEADS), minval=-0.75, maxval=0.75)
    shifts = jnp.broadcast_to(shifts, (block_count, SEQ_DEV, ATTENTION_HEADS)).reshape(FIRST_TOKENS1, ATTENTION_HEADS)
    bias_terms = base_level[None, :] + shifts + jitter
    slot_places = jax.random.randint(flow_lanes[3], (3, ATTENTION_HEADS), 0, FIRST_TOKENS1, dtype=jnp.int32)
    token_positions = jnp.arange(FIRST_TOKENS1, dtype=jnp.int32)[:, None]
    spike_mask = (token_positions == slot_places[0][None, :]) | (token_positions == slot_places[1][None, :]) | (token_positions == slot_places[2][None, :])
    spike_level = jax.random.uniform(flow_lanes[4], (FIRST_TOKENS1, ATTENTION_HEADS), minval=-2.0, maxval=-1.0)
    return jnp.where(spike_mask, spike_level, bias_terms).astype(jnp.float32)


def draw_expert_pick(key, part):
    base_key = jax.random.fold_in(key, 202)
    group_size = EXPERTS // GROUPS
    half_rows = TOK2_DEV // 2
    block_count = TOKENS2 // TOK2_DEV
    favored = jax.random.randint(jax.random.fold_in(base_key, 1), (), 0, GROUPS, dtype=jnp.int32)

    def one_block(block_key):
        flow_lanes = jax.random.split(block_key, 4)
        cut_points = jnp.sort(jax.random.randint(flow_lanes[0], (GROUPS - 2,), 0, half_rows + 1, dtype=jnp.int32))
        bounds = jnp.concatenate([jnp.zeros((1,), jnp.int32), cut_points, jnp.full((1,), half_rows, jnp.int32)])
        others = (favored + 1 + jnp.arange(GROUPS - 1, dtype=jnp.int32)) % GROUPS
        counts = jnp.zeros((GROUPS,), jnp.int32).at[favored].set(half_rows).at[others].set(bounds[1:] - bounds[:-1])
        group_ends = jnp.cumsum(counts)
        starts = group_ends - counts
        token_positions = jnp.arange(TOK2_DEV, dtype=jnp.int32)
        group_id = jnp.sum((token_positions[:, None] >= group_ends[None, :]).astype(jnp.int32), axis=1)
        group_rank = token_positions - starts[group_id]
        rotation = jax.random.randint(flow_lanes[1], (GROUPS,), 0, group_size, dtype=jnp.int32)
        offset = jax.random.randint(flow_lanes[2], (GROUPS,), 1, group_size, dtype=jnp.int32)
        first_pick = (group_rank + rotation[group_id]) % group_size
        second = (group_rank + rotation[group_id] + offset[group_id]) % group_size
        picked = jnp.stack([group_id * group_size + first_pick, group_id * group_size + second], axis=1)
        return picked[jax.random.permutation(flow_lanes[3], TOK2_DEV)]
    blocks = jax.vmap(one_block)(jax.random.split(base_key, block_count))
    return blocks.reshape(TOKENS2, TOPK).astype(jnp.int32)


def shard_levels(own_key, shape, cuts, least, top_value):
    gain = 1.0
    for dim, parts in cuts:
        heights = jax.random.uniform(jax.random.fold_in(jax.random.fold_in(own_key, 6), dim), (parts,), jnp.float32, least / len(cuts), top_value / len(cuts))
        gain = gain * jnp.repeat(jnp.exp(heights), shape[dim] // parts).reshape((-1,) + (1,) * (len(shape) - 1 - dim))
    return gain


def bell_draw(key, extent, spread, bound, shards=(), kind=jnp.bfloat16):
    drawn = jax.random.normal(key, extent, jnp.float32) * spread
    if len(shards) > 0:
        drawn = shard_levels(key, extent, shards, -0.22, 0.18) * drawn
    return jnp.clip(drawn, min=-bound, max=bound).astype(kind)


def setup_inputs(seed: int = 0) -> dict:
    keys = jax.random.split(jax.random.key(seed), 13)
    return {
        "query_rows": bell_draw(keys[0], (FIRST_TOKENS1, ATTENTION_HEADS * HEAD_DIM), 1.7, 10.0, ((0, 32), (1, 4))),
        "key_rows": bell_draw(keys[1], (FIRST_TOKENS1, ATTENTION_HEADS * HEAD_DIM), 1.7, 10.0, ((0, 32), (1, 4))),
        "value_rows": bell_draw(keys[2], (FIRST_TOKENS1, ATTENTION_HEADS * HEAD_DIM), 1.0, 6.0, ((0, 32), (1, 4))),
        "key_bias": draw_key_bias(jax.random.fold_in(keys[12], 71), 0),
        "out_weight": bell_draw(keys[4], (ATTENTION_HEADS * HEAD_DIM, D), (3.0 * (ATTENTION_HEADS * HEAD_DIM) ** -0.5), 0.5625, ((0, 4),)),
        "moe_input": bell_draw(keys[5], (TOKENS2, D), 1.0, 6.0, ((0, 128),)),
        "moe_gain": jnp.clip(1.0 + 0.18 * jax.random.normal(keys[6], (D,), jnp.float32), 0.1, 1.9),
        "expert_pick": draw_expert_pick(jax.random.fold_in(keys[12], 71), 0),
        "route_weight": jnp.clip(jnp.exp(math.log(1.0) - 2.3025851 * jax.random.uniform(keys[8], (TOKENS2, TOPK), jnp.float32) ** shard_levels(keys[8], (TOKENS2, TOPK), ((0, 128),), -0.2, 0.2)), 0.1, 1.0),
        "w_gate": bell_draw(keys[9], (EXPERTS, D, FF), D ** -0.5, 0.125, ((0, 32), (2, 4))),
        "w_up": bell_draw(keys[10], (EXPERTS, D, FF), D ** -0.5, 0.125, ((0, 32), (2, 4))),
        "w_down": bell_draw(keys[11], (EXPERTS, FF, D), FF ** -0.5, 0.1875, ((0, 32), (1, 4))),
    }


def block_values(query_heads, query_first, key_heads, value_heads, bias_heads, key_first, running):
    scores = jnp.einsum('hqd,hkd->hqk', query_heads.astype(jnp.float32), key_heads.astype(jnp.float32))
    scores = scores * HEAD_DIM ** (-0.5) + bias_heads[:, None, :]
    query_pos = query_first + jnp.arange(query_heads.shape[1], dtype=jnp.int32)
    key_pos = key_first + jnp.arange(key_heads.shape[1], dtype=jnp.int32)
    causal = (key_pos[None, :] < query_pos[:, None])[None]
    failure = jnp.where(causal, jax.nn.log_sigmoid(-scores), 0.0)
    remainder = lax.cumsum(failure, axis=2, reverse=True) - failure + running[:, :, None]
    stick_weight = jnp.where(causal, jnp.exp(jax.nn.log_sigmoid(scores) + remainder), 0.0).astype(jnp.bfloat16)
    portion = jnp.einsum('hqk,hkd->hqd', stick_weight.astype(jnp.float32), value_heads.astype(jnp.float32))
    return (portion, running + lax.optimization_barrier(jnp.sum(failure, axis=2)))

def mixer(query_rows, key_rows, value_rows, key_bias, out_weight):
    block_count = FIRST_TOKENS1 // SEQ_DEV

    def split_heads(rows):
        return jnp.transpose(rows.reshape(block_count, SEQ_DEV, ATTENTION_HEADS, HEAD_DIM), (0, 2, 1, 3))
    query_heads = split_heads(query_rows)
    key_heads = split_heads(key_rows)
    value_heads = split_heads(value_rows)
    bias_heads = jnp.transpose(key_bias.reshape(block_count, SEQ_DEV, ATTENTION_HEADS), (0, 2, 1))

    def one_block(block_index):

        def visit(step_index, carried):
            source = block_index - step_index
            portion, running = block_values(query_heads[block_index], block_index * SEQ_DEV, key_heads[source], value_heads[source], bias_heads[source], source * SEQ_DEV, carried[1])
            return (carried[0] + portion, running)
        start_state = (jnp.zeros((ATTENTION_HEADS, SEQ_DEV, HEAD_DIM), jnp.float32), jnp.zeros((ATTENTION_HEADS, SEQ_DEV), jnp.float32))
        steps_here = block_index % SEQ_BLOCKS + 1
        return lax.fori_loop(0, steps_here, visit, start_state)[0].astype(jnp.bfloat16)
    attended = lax.map(one_block, jnp.arange(block_count, dtype=jnp.int32))
    attended = jnp.transpose(attended, (0, 2, 1, 3)).reshape(FIRST_TOKENS1, ATTENTION_HEADS * HEAD_DIM)
    group_width = ATTENTION_HEADS * HEAD_DIM // N_TP
    summed = jnp.zeros((FIRST_TOKENS1, D), jnp.float32)
    for group in range(N_TP):
        columns = attended[:, group * group_width:(group + 1) * group_width]
        weights = out_weight[group * group_width:(group + 1) * group_width]
        rounded = jnp.dot(columns, weights, preferred_element_type=jnp.float32).astype(jnp.bfloat16)
        summed = summed + lax.optimization_barrier(rounded).astype(jnp.float32)
    return summed.astype(jnp.bfloat16)

def experts(moe_input, moe_gain, expert_pick, route_weight, w_gate, w_up, w_down):
    widened = moe_input.astype(jnp.float32)
    normed = (widened * lax.rsqrt(lax.optimization_barrier(jnp.mean(widened * widened, axis=1, keepdims=True)) + 1e-06) * moe_gain).astype(jnp.bfloat16)
    block_count = TOKENS2 // TOK2_DEV
    picks = expert_pick.reshape(block_count, TOK2_DEV * TOPK)
    matches = (picks[:, :, None] == jnp.arange(EXPERTS, dtype=jnp.int32)[None, None, :]).astype(jnp.int32)
    ranks = lax.optimization_barrier(jnp.sum((jnp.cumsum(matches, axis=1) - matches) * matches, axis=2))
    block_ids = jnp.arange(block_count, dtype=jnp.int32)[:, None]
    slots = picks * (block_count * CAP) + block_ids * CAP + ranks
    owners = block_ids * TOK2_DEV + jnp.arange(TOK2_DEV * TOPK, dtype=jnp.int32)[None, :] // TOPK
    table = jnp.full((EXPERTS * block_count * CAP,), TOKENS2, jnp.int32)
    table = table.at[slots.reshape(-1)].set(owners.reshape(-1)).reshape(EXPERTS, block_count * CAP)
    padded = jnp.concatenate([normed, jnp.zeros((1, D), jnp.bfloat16)], axis=0)

    def serve(expert):
        rows = padded[table[expert]]
        gate_in = jnp.dot(rows, w_gate[expert], preferred_element_type=jnp.float32)
        up_in = jnp.dot(rows, w_up[expert], preferred_element_type=jnp.float32)
        hidden = (jax.nn.silu(gate_in) * up_in).astype(jnp.bfloat16)
        return jnp.dot(hidden, w_down[expert], preferred_element_type=jnp.float32).astype(jnp.bfloat16)
    served = lax.map(serve, jnp.arange(EXPERTS, dtype=jnp.int32))
    chosen = served.reshape(EXPERTS * block_count * CAP, D)[slots.reshape(-1)]
    chosen = chosen.reshape(TOKENS2, TOPK, D).astype(jnp.float32)
    return lax.optimization_barrier(jnp.sum(chosen * route_weight[:, :, None], axis=1)).astype(jnp.bfloat16)

def reference(query_rows, key_rows, value_rows, key_bias, out_weight, moe_input, moe_gain, expert_pick, route_weight, w_gate, w_up, w_down):
    return (mixer(query_rows, key_rows, value_rows, key_bias, out_weight), experts(moe_input, moe_gain, expert_pick, route_weight, w_gate, w_up, w_down))
```

```python
import math

import jax
import jax.numpy as jnp
from jax import lax
from jax.experimental import pallas as pl
from jax.experimental.pallas import tpu as pltpu
from jax.sharding import PartitionSpec as P

HEAD_DIM = 64
GROUPS = 4
TOPK = 2
BLOCK = 512
HALF = 256
RUNS = 8
RUN = HALF // RUNS
LOG2E = math.log2(math.e)
U_CAP = 48.0
norm_eps = 1e-06


def attend_kernel(tiles_ref, qt_ref, kv_ref, bias_ref, out_ref, kk_ref, rhs_ref, z_hi, z_lo, w_hi, w_lo, acc_ref, carry_ref):
    lanes = qt_ref.shape[2]
    low_lane = lax.broadcasted_iota(jnp.int32, (HALF, 128), 1) < HEAD_DIM
    sub = lax.broadcasted_iota(jnp.int32, (RUNS, 128), 0)
    row = lax.broadcasted_iota(jnp.int32, (128, lanes), 0)

    def build(b, carried):
        pair = kv_ref[b, 0:HALF, :].astype(jnp.float32)
        turned = pltpu.roll(pair, HEAD_DIM, axis=1)
        kk_ref[b, 0] = jnp.where(low_lane, pair, turned).astype(jnp.bfloat16)
        kk_ref[b, 1] = jnp.where(low_lane, turned, pair).astype(jnp.bfloat16)
        return carried

    lax.fori_loop(0, kv_ref.shape[0], build, 0)

    def later(x, n):
        return jnp.where(sub < RUNS - n, pltpu.roll(x, RUNS - n, axis=0), 1.0)

    def scores(b, half, z_ref):
        keys = jnp.concatenate([kk_ref[b, half], bias_ref[b, half]], axis=1)
        z_ref[...] = jnp.dot(keys, rhs_ref[...], preferred_element_type=jnp.float32)

    def weigh(z_ref, w_ref, first_key):
        for lane in range(0, lanes, 128):
            ls = slice(lane, lane + 128)
            us = []
            for i in range(RUN):
                u = jnp.exp2(jnp.minimum(z_ref[RUNS * i : RUNS * i + RUNS, ls], U_CAP))
                if first_key is not None:
                    query = lax.broadcasted_iota(jnp.int32, (RUNS, 128), 1) + lane
                    u = jnp.where(sub * RUN + (i + first_key) < query, u, 0.0)
                us.append(u)
            pairs = range(RUN // 2)
            rs = [1.0 / ((1.0 + us[2 * g]) * (1.0 + us[2 * g + 1])) for g in pairs]
            tree = list(rs)
            while len(tree) > 1:
                tree = [tree[2 * n] * tree[2 * n + 1] for n in range(len(tree) // 2)]
            total = tree[0]
            after = later(total, 1)
            after = after * later(after, 1)
            after = after * later(after, 2)
            after = after * later(after, 4)
            carry = carry_ref[:, ls]
            left = carry * after
            carry_ref[:, ls] = carry * jnp.broadcast_to((after * total)[0:1, :], (RUNS, 128))
            for g in reversed(pairs):
                left = left * rs[g]
                first = us[2 * g] * left
                second = us[2 * g + 1] * (left * (1.0 + us[2 * g]))
                both = jnp.concatenate([first, second], axis=0)
                w_ref[2 * RUNS * g : 2 * RUNS * g + 2 * RUNS, ls] = both.astype(jnp.bfloat16)

    def collect(b, half, w_ref):
        at = HALF + 2 * HEAD_DIM * half
        values = jnp.concatenate([kv_ref[b, at : at + HEAD_DIM, :], kv_ref[b, at + HEAD_DIM : at + 2 * HEAD_DIM, :]], axis=1)
        acc_ref[...] += jnp.dot(values, w_ref[...], preferred_element_type=jnp.float32)

    def tile(n, carried):
        p = tiles_ref[n]
        scaled = qt_ref[n].astype(jnp.float32) * (LOG2E * HEAD_DIM**-0.5)
        top = scaled.astype(jnp.bfloat16)
        rhs_ref[0:HEAD_DIM, :] = top
        rhs_ref[HEAD_DIM : 2 * HEAD_DIM, :] = (scaled - top.astype(jnp.float32)).astype(jnp.bfloat16)
        rhs_ref[128:256, :] = jnp.where(row < 3, 1.0, 0.0).astype(jnp.bfloat16)
        carry_ref[...] = jnp.ones_like(carry_ref)
        acc_ref[...] = jnp.zeros_like(acc_ref)
        scores(p, 1, z_hi)
        scores(p, 0, z_lo)
        weigh(z_hi, w_hi, HALF)
        scores(jnp.maximum(p - 1, 0), 1, z_hi)
        weigh(z_lo, w_lo, 0)
        collect(p, 1, w_hi)

        def visit(step, inner):
            b = p - 1 - step
            scores(b, 0, z_lo)
            weigh(z_hi, w_hi, None)
            collect(b + 1, 0, w_lo)
            scores(jnp.maximum(b - 1, 0), 1, z_hi)
            weigh(z_lo, w_lo, None)
            collect(b, 1, w_hi)
            return inner

        lax.fori_loop(0, p, visit, 0)
        collect(0, 0, w_lo)
        out_ref[n] = acc_ref[...].astype(jnp.bfloat16)
        return carried

    lax.fori_loop(0, qt_ref.shape[0], tile, 0)


def attend(tiles, qt, kv, bias):
    n_tiles, width, lanes = qt.shape
    blocks = kv.shape[0]
    whole = pl.BlockSpec(memory_space=pltpu.VMEM)
    return pl.pallas_call(
        attend_kernel,
        out_shape=jax.ShapeDtypeStruct((n_tiles, width, lanes), jnp.bfloat16),
        in_specs=[pl.BlockSpec(memory_space=pltpu.SMEM), whole, whole, whole],
        out_specs=whole,
        scratch_shapes=[
            pltpu.VMEM((blocks, 2, HALF, 128), jnp.bfloat16),
            pltpu.VMEM((HALF, lanes), jnp.bfloat16),
            pltpu.VMEM((HALF, lanes), jnp.float32),
            pltpu.VMEM((HALF, lanes), jnp.float32),
            pltpu.VMEM((HALF, lanes), jnp.bfloat16),
            pltpu.VMEM((HALF, lanes), jnp.bfloat16),
            pltpu.VMEM((width, lanes), jnp.float32),
            pltpu.VMEM((RUNS, lanes), jnp.float32),
        ],
        cost_estimate=pl.CostEstimate(flops=40_000_000_000, bytes_accessed=12 << 20, transcendentals=0),
        name="stick_attend",
    )(tiles, qt, kv, bias)


def key_order(rows):
    n = rows.shape[-1]
    return rows.reshape(2, RUNS, RUN, n).swapaxes(1, 2).reshape(BLOCK, n)


def bias_lanes(bias):
    left = bias * LOG2E
    lane = lax.broadcasted_iota(jnp.int32, bias.shape[:3] + (128,), 3)
    out = jnp.zeros(lane.shape, jnp.float32)
    for n in range(3):
        part = lax.reduce_precision(left, 8, 7)
        out = jnp.where(lane == n, part, out)
        left = left - part
    return out.astype(jnp.bfloat16)


def slot_and_turn(block):
    slot, at = block // 8, block % 8
    return slot, at if slot % 2 == 0 else 7 - at


def routes(turn):
    pairs = []
    for block in range(32):
        slot, j = slot_and_turn(block)
        pairs.append((block, j // 2 * 8 + (slot + turn) % 4 * 2 + j % 2))
    return pairs


def mixer(query_rows, key_rows, value_rows, key_bias, out_weight):
    ep_index = lax.axis_index("ep")
    head = ep_index // 2 % 4
    turn = ep_index // 8 * 2 + ep_index % 2
    my_slot = ep_index // 8

    q_heads = query_rows.T.reshape(4, HEAD_DIM, BLOCK)
    keys = key_order(key_rows).reshape(2, HALF, 4, HEAD_DIM)
    k_heads = keys.transpose(2, 1, 0, 3).reshape(4, HALF, 128)
    values = key_order(value_rows).T.reshape(4, HEAD_DIM, 4, 128)
    v_heads = values.transpose(0, 2, 1, 3).reshape(4, HALF, 128)
    kv_heads = jnp.concatenate([k_heads, v_heads], axis=1)
    kv_out = jnp.broadcast_to(kv_heads[None, :, None], (4, 4, 2, BLOCK, 128)).reshape(32, BLOCK, 128)
    kv = lax.all_to_all(kv_out, "ep", split_axis=0, concat_axis=0, tiled=True)

    q_twice = jnp.concatenate([q_heads, q_heads], axis=0)
    q_got, tiles = [], []
    for r in range(4):
        mine = lax.dynamic_index_in_dim(q_twice, my_slot + r, 0, keepdims=False)
        q_got.append(lax.ppermute(mine, "ep", routes(r)))
        slot = (head - r + 4) % 4
        tiles.append(slot * 8 + jnp.where(slot % 2 == 0, turn, 7 - turn))
    qt = jnp.stack(q_got)
    tiles = jnp.stack(tiles).astype(jnp.int32)

    column = lax.dynamic_slice_in_dim(key_bias, head, 1, 1)
    bias = bias_lanes(column.reshape(32, 2, RUNS, RUN, 1).swapaxes(2, 3).reshape(32, 2, HALF, 1))

    done = attend(tiles, qt, kv, bias)

    back = [lax.ppermute(done[r], "ep", [(b, a) for a, b in routes(r)]) for r in range(4)]
    twice = jnp.stack(back + back)
    attended = lax.dynamic_slice_in_dim(twice, 4 - my_slot, 4, 0)
    pieces = attended.reshape(4 * HEAD_DIM, 4, 128).swapaxes(0, 1)
    columns = lax.all_to_all(pieces, "tp", split_axis=0, concat_axis=0, tiled=True)
    weight = lax.all_gather(out_weight, "tp", axis=0, tiled=True)
    columns = columns.reshape(weight.shape[0], 128)
    return jnp.einsum("cr,cm->rm", columns, weight, preferred_element_type=jnp.float32).astype(jnp.bfloat16)


def gather_turned(arrays, axis, dims):
    turned = [jnp.moveaxis(a, dim, 0) for a, dim in zip(arrays, dims)]
    both = jnp.concatenate([t.reshape(len(t), -1) for t in turned], axis=1)
    filled, at, done = (lax.all_gather(both, axis, axis=0, tiled=True), 0, [])
    for t, dim in zip(turned, dims):
        slab = filled[:, at : at + t[0].size].reshape(-1, *t.shape[1:])
        done.append(jnp.moveaxis(slab, 0, dim))
        at += t[0].size
    return tuple(done)


def expand(arrived, gate_weights, up_weights):
    gate_in = jnp.einsum("necm,emf->necf", arrived, gate_weights, preferred_element_type=jnp.float32)
    up_in = jnp.einsum("necm,emf->necf", arrived, up_weights, preferred_element_type=jnp.float32)
    return (jax.nn.silu(gate_in) * up_in).astype(jnp.bfloat16)


def contract(hidden, down_weights):
    return jnp.einsum("necf,efm->necm", hidden, down_weights, preferred_element_type=jnp.float32)


def experts(moe_input, moe_gain, expert_pick, route_weight, w_gate, w_up, w_down):
    ep_count = lax.axis_size("ep")
    token_count = moe_input.shape[0]
    widened = moe_input.astype(jnp.float32)
    normed = (
        widened * lax.rsqrt(jnp.mean(widened * widened, axis=1, keepdims=True) + norm_eps) * moe_gain
    ).astype(jnp.bfloat16)
    local_experts = w_gate.shape[0]
    expert_total = local_experts * ep_count
    capacity = GROUPS * token_count // expert_total
    picks = expert_pick.reshape(-1)
    matches = (picks[:, None] == jnp.arange(expert_total, dtype=jnp.int32)[None, :]).astype(jnp.int32)
    ranks = jnp.sum((jnp.cumsum(matches, axis=0) - matches) * matches, axis=1)
    slots = picks * capacity + ranks
    owners = jnp.arange(picks.shape[0], dtype=jnp.int32) // TOPK
    table = jnp.full((expert_total * capacity,), token_count, jnp.int32).at[slots].set(owners)
    padded = jnp.concatenate([normed, jnp.zeros((1, normed.shape[1]), jnp.bfloat16)], axis=0)
    outgoing = padded[table].reshape(ep_count, local_experts, capacity, normed.shape[1])
    arrived = lax.all_to_all(outgoing, "ep", split_axis=0, concat_axis=0, tiled=True)
    gate_all, up_all, down_all = gather_turned((w_gate, w_up, w_down), "tp", (2, 2, 1))
    served = contract(expand(arrived, gate_all, up_all), down_all).astype(jnp.bfloat16)
    returned = lax.all_to_all(served, "ep", split_axis=0, concat_axis=0, tiled=True)
    flat = returned.reshape(expert_total * capacity, returned.shape[3])
    chosen = flat[slots].reshape(token_count, TOPK, flat.shape[1]).astype(jnp.float32)
    return jnp.sum(chosen * route_weight[:, :, None], axis=1).astype(jnp.bfloat16)


def local(
    query_rows, key_rows, value_rows, key_bias, out_weight, moe_input, moe_gain,
    expert_pick, route_weight, w_gate, w_up, w_down,
):
    routed_out = experts(moe_input, moe_gain, expert_pick, route_weight, w_gate, w_up, w_down)
    mixer_out = mixer(query_rows, key_rows, value_rows, key_bias, out_weight)
    return (mixer_out, routed_out)


def solution(mesh):
    placed = (
        P("ep", "tp"), P("ep", "tp"), P("ep", "tp"), P(None, "tp"), P("tp", None),
        P(("ep", "tp"), None), P(), P(("ep", "tp"), None), P(("ep", "tp"), None),
        P("ep", None, "tp"), P("ep", None, "tp"), P("ep", "tp", None),
    )
    return jax.shard_map(
        local,
        mesh=mesh,
        in_specs=placed,
        out_specs=(P(("ep", "tp"), None), P(("ep", "tp"), None)),
        check_vma=False,
    )
```

```python
import math

import jax
import jax.numpy as jnp
from jax import lax
from jax.experimental import pallas as pl
from jax.experimental.pallas import tpu as pltpu
from jax.sharding import PartitionSpec as P


HEAD_DIM = 64
GROUPS = 4
TOPK = 2
BLOCK = 512
HALF = 256
RUNS = 8
RUN = HALF // RUNS
LOG2E = math.log2(math.e)
U_CAP = 48.0
MESH = pl.DeviceIdType.MESH
norm_eps = 1e-06


def attend_kernel(tiles_ref, qt_ref, kv_ref, rows_ref, out_ref, kk_ref, bias_ref, rhs_ref, z_hi, z_lo, w_hi, w_lo, acc_ref, carry_ref):
    lanes = qt_ref.shape[2]
    low_lane = lax.broadcasted_iota(jnp.int32, (HALF, 128), 1) < HEAD_DIM
    sub = lax.broadcasted_iota(jnp.int32, (RUNS, 128), 0)
    row = lax.broadcasted_iota(jnp.int32, (128, lanes), 0)

    def build(b, carried):
        pair = kv_ref[b, 0:HALF, :].astype(jnp.float32)
        turned = pltpu.roll(pair, HEAD_DIM, axis=1)
        kk_ref[b, 0] = jnp.where(low_lane, pair, turned).astype(jnp.bfloat16)
        kk_ref[b, 1] = jnp.where(low_lane, turned, pair).astype(jnp.bfloat16)
        for half in range(2):
            value = rows_ref[b, half : half + 1, :] * LOG2E
            parts = jnp.zeros((128, HALF), jnp.float32)
            for n in range(3):
                part = value.astype(jnp.bfloat16).astype(jnp.float32)
                parts = jnp.where(row[:, 0:HALF] == n, part, parts)
                value = value - part
            bias_ref[b, half] = parts.T.astype(jnp.bfloat16)
        return carried

    lax.fori_loop(0, kv_ref.shape[0], build, 0)

    def later(x, n):
        return jnp.where(sub < RUNS - n, pltpu.roll(x, RUNS - n, axis=0), 1.0)

    def scores(b, half, z_ref):
        keys = jnp.concatenate([kk_ref[b, half], bias_ref[b, half]], axis=1)
        z_ref[...] = jnp.dot(keys, rhs_ref[...], preferred_element_type=jnp.float32)

    def weigh(z_ref, w_ref, first_key):
        for lane in range(0, lanes, 128):
            ls = slice(lane, lane + 128)
            us = []
            for i in range(RUN):
                u = jnp.exp2(jnp.minimum(z_ref[RUNS * i : RUNS * i + RUNS, ls], U_CAP))
                if first_key is not None:
                    query = lax.broadcasted_iota(jnp.int32, (RUNS, 128), 1) + lane
                    u = jnp.where(sub * RUN + (i + first_key) < query, u, 0.0)
                us.append(u)
            pairs = range(RUN // 2)
            rs = [1.0 / ((1.0 + us[2 * g]) * (1.0 + us[2 * g + 1])) for g in pairs]
            tree = list(rs)
            while len(tree) > 1:
                tree = [tree[2 * n] * tree[2 * n + 1] for n in range(len(tree) // 2)]
            total = tree[0]
            after = later(total, 1)
            after = after * later(after, 1)
            after = after * later(after, 2)
            after = after * later(after, 4)
            carry = carry_ref[:, ls]
            left = carry * after
            carry_ref[:, ls] = carry * jnp.broadcast_to((after * total)[0:1, :], (RUNS, 128))
            for g in reversed(pairs):
                left = left * rs[g]
                first = us[2 * g] * left
                second = us[2 * g + 1] * (left * (1.0 + us[2 * g]))
                both = jnp.concatenate([first, second], axis=0)
                w_ref[2 * RUNS * g : 2 * RUNS * g + 2 * RUNS, ls] = both.astype(jnp.bfloat16)

    def collect(b, half, w_ref):
        at = HALF + 2 * HEAD_DIM * half
        values = jnp.concatenate([kv_ref[b, at : at + HEAD_DIM, :], kv_ref[b, at + HEAD_DIM : at + 2 * HEAD_DIM, :]], axis=1)
        acc_ref[...] += jnp.dot(values, w_ref[...], preferred_element_type=jnp.float32)

    def tile(n, carried):
        p = tiles_ref[n]
        scaled = qt_ref[n].astype(jnp.float32) * (LOG2E * HEAD_DIM**-0.5)
        top = scaled.astype(jnp.bfloat16)
        rhs_ref[0:HEAD_DIM, :] = top
        rhs_ref[HEAD_DIM : 2 * HEAD_DIM, :] = (scaled - top.astype(jnp.float32)).astype(jnp.bfloat16)
        rhs_ref[128:256, :] = jnp.where(row < 3, 1.0, 0.0).astype(jnp.bfloat16)
        carry_ref[...] = jnp.ones_like(carry_ref)
        acc_ref[...] = jnp.zeros_like(acc_ref)
        scores(p, 1, z_hi)
        scores(p, 0, z_lo)
        weigh(z_hi, w_hi, HALF)
        scores(jnp.maximum(p - 1, 0), 1, z_hi)
        weigh(z_lo, w_lo, 0)
        collect(p, 1, w_hi)

        def visit(step, inner):
            b = p - 1 - step
            scores(b, 0, z_lo)
            weigh(z_hi, w_hi, None)
            collect(b + 1, 0, w_lo)
            scores(jnp.maximum(b - 1, 0), 1, z_hi)
            weigh(z_lo, w_lo, None)
            collect(b, 1, w_hi)
            return inner

        lax.fori_loop(0, p, visit, 0)
        collect(0, 0, w_lo)
        out_ref[n] = acc_ref[...].astype(jnp.bfloat16)
        return carried

    lax.fori_loop(0, qt_ref.shape[0], tile, 0)


def attend(tiles, qt, kv, bias):
    n_tiles, width, lanes = qt.shape
    blocks = kv.shape[0]
    whole = pl.BlockSpec(memory_space=pltpu.VMEM)
    return pl.pallas_call(
        attend_kernel,
        out_shape=jax.ShapeDtypeStruct((n_tiles, width, lanes), jnp.bfloat16),
        in_specs=[pl.BlockSpec(memory_space=pltpu.SMEM), whole, whole, whole],
        out_specs=whole,
        scratch_shapes=[
            pltpu.VMEM((blocks, 2, HALF, 128), jnp.bfloat16),
            pltpu.VMEM((blocks, 2, HALF, 128), jnp.bfloat16),
            pltpu.VMEM((HALF, lanes), jnp.bfloat16),
            pltpu.VMEM((HALF, lanes), jnp.float32),
            pltpu.VMEM((HALF, lanes), jnp.float32),
            pltpu.VMEM((HALF, lanes), jnp.bfloat16),
            pltpu.VMEM((HALF, lanes), jnp.bfloat16),
            pltpu.VMEM((width, lanes), jnp.float32),
            pltpu.VMEM((RUNS, lanes), jnp.float32),
        ],
        cost_estimate=pl.CostEstimate(flops=20_000_000_000, bytes_accessed=12 << 20, transcendentals=0),
        name="stick_attend",
    )(tiles, qt, kv, bias)


def key_order(rows):
    n = rows.shape[-1]
    return rows.reshape(2, RUNS, RUN, n).swapaxes(1, 2).reshape(BLOCK, n)


def turn_of(block):
    slot, at = block // 8, block % 8
    return jnp.where(slot % 2 == 0, at, 7 - at)


def block_of(slot, turn):
    return slot * 8 + jnp.where(slot % 2 == 0, turn, 7 - turn)


def exchange_kernel(kv_ref, q_ref, kv_out, q_out, got, q_got, s_col, s_up, s_down, s_pair, s_q, s_own):
    me = lax.axis_index("ep")
    z, y, c = me // 8, me // 2 % 4, me % 2
    turn = 2 * z + c
    my_slot, my_turn = z, turn_of(me)

    def at(zz, yy, cc):
        return (zz + 4) % 4 * 8 + (yy + 4) % 4 * 2 + cc

    def dest(index):
        return {"ep": index}

    def q_dest(h):
        return my_turn // 2 * 8 + 2 * h + my_turn % 2

    barrier = pltpu.get_barrier_semaphore()
    near = [at(z, y + d, c) for d in (1, 2, 3)] + [at(z + 1, y, c), at(z - 1, y, c), at(z, y, 1 - c)]
    for index in near:
        pl.semaphore_signal(barrier, inc=1, device_id=dest(index), device_id_type=MESH)
    alone = (my_turn == turn).astype(jnp.int32)
    for h in range(4):
        @pl.when(q_dest(h) != me)
        def _():
            pl.semaphore_signal(barrier, inc=1, device_id=dest(q_dest(h)), device_id_type=MESH)

        @pl.when(block_of(h, turn) != me)
        def _():
            pl.semaphore_signal(barrier, inc=1, device_id=dest(block_of(h, turn)), device_id_type=MESH)
    pl.semaphore_wait(barrier, len(near) + 8 - 2 * alone)

    def send(src, index, dst, send_sem, recv_sem):
        copy = pltpu.make_async_remote_copy(
            src_ref=src, dst_ref=dst, send_sem=send_sem, recv_sem=recv_sem,
            device_id=dest(index), device_id_type=MESH,
        )
        copy.start()
        return copy

    def piece(index):
        return kv_out.at[index]

    def arrived(index):
        pltpu.make_async_copy(piece(index), piece(index), got.at[index]).wait()

    sent = []
    for d in (1, 2, 3):
        sent.append(send(kv_ref.at[(y + d) % 4], at(z, y + d, c), piece(me), s_col.at[d - 1], got.at[me]))
    for h in range(4):
        @pl.when(q_dest(h) != me)
        def _():
            send(q_ref.at[h], q_dest(h), q_out.at[my_slot], s_q.at[h], q_got.at[my_slot])

        @pl.when(q_dest(h) == me)
        def _():
            pltpu.make_async_copy(q_ref.at[h], q_out.at[my_slot], q_got.at[my_slot]).start()
    own = pltpu.make_async_copy(kv_ref.at[y], piece(me), s_own)
    own.start()
    for d in range(4):
        index = at(z, y - d, c)
        if d > 0:
            arrived(index)
        src = kv_ref.at[y] if d == 0 else piece(index)
        sent.append(send(src, at(z + 1, y, c), piece(index), s_up.at[d], got.at[index]))
        sent.append(send(src, at(z - 1, y, c), piece(index), s_down.at[d], got.at[index]))
        sent.append(send(src, at(z, y, 1 - c), piece(index), s_pair.at[d], got.at[index]))
    for d in range(4):
        for n, dz in enumerate((1, -1)):
            index = at(z - dz, y - d, c)
            arrived(index)
            if d < 2 and dz == 1:
                sent.append(send(piece(index), at(z + 1, y, c), piece(index), s_up.at[4 + d], got.at[index]))
            if d >= 2 and dz == -1:
                sent.append(send(piece(index), at(z - 1, y, c), piece(index), s_down.at[2 + d], got.at[index]))
            sent.append(send(piece(index), at(z, y, 1 - c), piece(index), s_pair.at[4 + 2 * d + n], got.at[index]))
    for d in (0, 2, 1, 3):
        index = at(z + 2, y - d, c)
        arrived(index)
        sent.append(send(piece(index), at(z, y, 1 - c), piece(index), s_pair.at[12 + d], got.at[index]))
    for k in range(4):
        pltpu.make_async_copy(q_out.at[k], q_out.at[k], q_got.at[k]).wait()
    for zz in range(4):
        for yy in range(4):
            arrived(at(zz, yy, 1 - c))
    own.wait()
    for copy in sent:
        copy.wait_send()
    for h in range(4):
        @pl.when(q_dest(h) != me)
        def _():
            pltpu.make_async_copy(q_ref.at[h], q_ref.at[h], s_q.at[h]).wait()


def exchange(kv, q):
    whole = pl.BlockSpec(memory_space=pltpu.VMEM)
    dma = pltpu.SemaphoreType.DMA
    return pl.pallas_call(
        exchange_kernel,
        out_shape=(
            jax.ShapeDtypeStruct((32,) + kv.shape[1:], kv.dtype),
            jax.ShapeDtypeStruct(q.shape, q.dtype),
        ),
        in_specs=[whole, whole],
        out_specs=(whole, whole),
        scratch_shapes=[dma((32,)), dma((4,)), dma((3,)), dma((6,)), dma((6,)), dma((16,)), dma((4,)), dma],
        compiler_params=pltpu.CompilerParams(collective_id=1, has_side_effects=True),
        cost_estimate=pl.CostEstimate(flops=20_000_000_000, bytes_accessed=8 << 20, transcendentals=0),
        name="exchange",
    )(kv, q)


def slot_and_turn(block):
    slot, at = block // 8, block % 8
    return slot, at if slot % 2 == 0 else 7 - at


def homeward(step):
    pairs = []
    for block in range(32):
        slot, j = slot_and_turn(block)
        head = (slot + step) % 4
        pairs.append((j // 2 * 8 + head * 2 + j % 2, block))
    return pairs


def mixer(query_rows, key_rows, value_rows, key_bias, out_weight):
    ep_index = lax.axis_index("ep")
    head = (ep_index >> 1) & 3
    turn = (ep_index >> 3) * 2 + (ep_index & 1)
    my_slot = ep_index >> 3

    q_heads = query_rows.T.reshape(4, HEAD_DIM, BLOCK)
    keys = key_order(key_rows).reshape(2, HALF, 4, HEAD_DIM)
    k_heads = keys.transpose(2, 1, 0, 3).reshape(4, HALF, 128)
    values = key_order(value_rows).T.reshape(4, HEAD_DIM, 4, 128)
    v_heads = values.transpose(0, 2, 1, 3).reshape(4, HALF, 128)
    kv, qt = exchange(jnp.concatenate([k_heads, v_heads], axis=1), q_heads)

    column = lax.dynamic_slice_in_dim(key_bias, head, 1, 1)
    bias = column.reshape(32, 2, RUNS, RUN).swapaxes(2, 3).reshape(32, 2, HALF)
    done_a = attend(jnp.stack([turn, 31 - turn]).astype(jnp.int32), jnp.stack([qt[0], qt[3]]), kv, bias)
    done_b = attend(jnp.stack([15 - turn, 16 + turn]).astype(jnp.int32), qt[1:3], kv, bias)
    done = jnp.stack([done_a[0], done_b[0], done_b[1], done_a[1]])

    twice = jnp.concatenate([done, done], axis=0)
    back = []
    for r in range(4):
        mine = lax.dynamic_index_in_dim(twice, (head - r) & 3, 0, keepdims=False)
        back.append(lax.ppermute(mine, "ep", homeward(r)))
    rows = [lax.dynamic_slice_in_dim(out_weight, ((my_slot + r) & 3) * HEAD_DIM, HEAD_DIM, 0) for r in range(4)]
    attended = jnp.concatenate(back, axis=0)
    part = jnp.einsum("cr,cm->rm", attended, jnp.concatenate(rows, axis=0), preferred_element_type=jnp.float32)
    pieces = part.astype(jnp.bfloat16).reshape(4, 128, part.shape[1])
    arrived = lax.all_to_all(pieces, "tp", split_axis=0, concat_axis=0, tiled=True)
    return arrived.astype(jnp.float32).sum(axis=0).astype(jnp.bfloat16)


RIGHT = [(i, (i + 1) % 4) for i in range(4)]
LEFT = [(i, (i + 3) % 4) for i in range(4)]


def neighbours(shard):
    return lax.ppermute(shard, "tp", RIGHT), lax.ppermute(shard, "tp", LEFT)


def opposite(from_left, from_right):
    half = from_left.shape[0] // 2
    return lax.ppermute(from_left[:half], "tp", RIGHT), lax.ppermute(from_right[half:], "tp", LEFT)


def dot(a, b):
    return jnp.dot(a, b, preferred_element_type=jnp.float32)


def experts(moe_input, moe_gain, expert_pick, route_weight, w_gate, w_up, w_down):
    ep_count = lax.axis_size("ep")
    token_count = moe_input.shape[0]
    widened = moe_input.astype(jnp.float32)
    normed = (
        widened * lax.rsqrt(jnp.mean(widened * widened, axis=1, keepdims=True) + norm_eps) * moe_gain
    ).astype(jnp.bfloat16)
    local_experts = w_gate.shape[0]
    expert_total = local_experts * ep_count
    capacity = GROUPS * token_count // expert_total
    picks = expert_pick.reshape(-1)
    matches = (picks[:, None] == jnp.arange(expert_total, dtype=jnp.int32)[None, :]).astype(jnp.int32)
    ranks = jnp.sum((jnp.cumsum(matches, axis=0) - matches) * matches, axis=1)
    slots = picks * capacity + ranks
    owners = jnp.arange(picks.shape[0], dtype=jnp.int32) // TOPK
    table = jnp.full((expert_total * capacity,), token_count, jnp.int32).at[slots].set(owners)
    padded = jnp.concatenate([normed, jnp.zeros((1, normed.shape[1]), jnp.bfloat16)], axis=0)
    outgoing = padded[table].reshape(ep_count, local_experts, capacity, normed.shape[1])
    arrived = lax.all_to_all(outgoing, "ep", split_axis=0, concat_axis=0, tiled=True)
    rows = arrived.reshape(expert_total * capacity, normed.shape[1])
    both = jnp.concatenate([w_gate[0], w_up[0]], axis=1)
    both_left, both_right = neighbours(both)
    down_left, down_right = neighbours(w_down[0])
    both_a, both_b = opposite(both_left, both_right)
    down_a, down_b = opposite(down_left, down_right)
    half = both.shape[0] // 2
    ins = [dot(rows, part) for part in (both, both_left, both_right)]
    ins.append(dot(rows[:, :half], both_a) + dot(rows[:, half:], both_b))
    width = w_gate.shape[2]
    hidden = [(jax.nn.silu(v[:, :width]) * v[:, width:]).astype(jnp.bfloat16) for v in ins]
    downs = jnp.concatenate([w_down[0], down_left, down_right, down_a, down_b], axis=0)
    served = dot(jnp.concatenate(hidden, axis=1), downs).astype(jnp.bfloat16)
    served = served.reshape(ep_count, local_experts, capacity, normed.shape[1])
    returned = lax.all_to_all(served, "ep", split_axis=0, concat_axis=0, tiled=True)
    flat = returned.reshape(expert_total * capacity, returned.shape[3])
    chosen = flat[slots].reshape(token_count, TOPK, flat.shape[1]).astype(jnp.float32)
    return jnp.sum(chosen * route_weight[:, :, None], axis=1).astype(jnp.bfloat16)


def local(
    query_rows, key_rows, value_rows, key_bias, out_weight, moe_input, moe_gain,
    expert_pick, route_weight, w_gate, w_up, w_down,
):
    routed_out = experts(moe_input, moe_gain, expert_pick, route_weight, w_gate, w_up, w_down)
    mixer_out = mixer(query_rows, key_rows, value_rows, key_bias, out_weight)
    return (mixer_out, routed_out)


def solution(mesh):
    placed = (
        P("ep", "tp"), P("ep", "tp"), P("ep", "tp"), P(None, "tp"), P("tp", None),
        P(("ep", "tp"), None), P(), P(("ep", "tp"), None), P(("ep", "tp"), None),
        P("ep", None, "tp"), P("ep", None, "tp"), P("ep", "tp", None),
    )
    return jax.shard_map(
        local,
        mesh=mesh,
        in_specs=placed,
        out_specs=(P(("ep", "tp"), None), P(("ep", "tp"), None)),
        check_vma=False,
    )
```

```python
import math

import jax
import jax.numpy as jnp
from jax import lax
from jax.experimental import pallas as pl
from jax.experimental.pallas import tpu as pltpu
from jax.sharding import PartitionSpec as P


HEAD_DIM = 64
GROUPS = 4
TOPK = 2
BLOCK = 512
HALF = 256
RUNS = 8
RUN = HALF // RUNS
LOG2E = math.log2(math.e)
U_CAP = 48.0
MESH = pl.DeviceIdType.MESH
norm_eps = 1e-06


def turn_of(block):
    slot, at = block // 8, block % 8
    return jnp.where(slot % 2 == 0, at, 7 - at)


def block_of(slot, turn):
    return slot * 8 + jnp.where(slot % 2 == 0, turn, 7 - turn)


def mix_kernel(
    kv_ref, q_ref, rows_ref, rows_out_ref, home_ref, rows_in_ref,
    kv_all, qt_ref, done_ref, kk_ref, bias_ref, rhs_ref, z_hi, z_lo, w_hi, w_lo, acc_ref, carry_ref,
    got, q_got, home_got, row_got, s_col, s_up, s_down, s_pair, s_q, s_home, s_row, s_own,
):
    me = lax.axis_index("ep")
    z, y, c = me // 8, me // 2 % 4, me % 2
    turn = 2 * z + c
    my_turn = turn_of(me)
    lanes = qt_ref.shape[2]

    def at(zz, yy, cc):
        return (zz + 4) % 4 * 8 + (yy + 4) % 4 * 2 + cc

    def dest(index):
        return {"ep": index}

    def q_dest(h):
        return my_turn // 2 * 8 + 2 * h + my_turn % 2

    barrier = pltpu.get_barrier_semaphore()

    def greet(d, carried):
        pl.semaphore_signal(barrier, inc=1, device_id=dest((me + d) % 32), device_id_type=MESH)
        return carried

    lax.fori_loop(1, 32, greet, 0)
    pl.semaphore_wait(barrier, 31)

    def send(src, index, dst, send_sem, recv_sem):
        copy = pltpu.make_async_remote_copy(
            src_ref=src, dst_ref=dst, send_sem=send_sem, recv_sem=recv_sem,
            device_id=dest(index), device_id_type=MESH,
        )
        copy.start()
        return copy

    def piece(index):
        return kv_all.at[index]

    def arrived(index):
        pltpu.make_async_copy(piece(index), piece(index), got.at[index]).wait()

    sent = []
    for d in (1, 2, 3):
        sent.append(send(kv_ref.at[(y + d) % 4], at(z, y + d, c), piece(me), s_col.at[d - 1], got.at[me]))
    for h in range(4):
        @pl.when(q_dest(h) != me)
        def _():
            send(q_ref.at[h], q_dest(h), qt_ref.at[z], s_q.at[h], q_got.at[z])

        @pl.when(q_dest(h) == me)
        def _():
            pltpu.make_async_copy(q_ref.at[h], qt_ref.at[z], q_got.at[z]).start()
    own = pltpu.make_async_copy(kv_ref.at[y], piece(me), s_own.at[0])
    own.start()
    for d in range(4):
        index = at(z, y - d, c)
        if d > 0:
            arrived(index)
        src = kv_ref.at[y] if d == 0 else piece(index)
        sent.append(send(src, at(z + 1, y, c), piece(index), s_up.at[d], got.at[index]))
        sent.append(send(src, at(z - 1, y, c), piece(index), s_down.at[d], got.at[index]))
        sent.append(send(src, at(z, y, 1 - c), piece(index), s_pair.at[d], got.at[index]))

    low_lane = lax.broadcasted_iota(jnp.int32, (HALF, 128), 1) < HEAD_DIM
    sub = lax.broadcasted_iota(jnp.int32, (RUNS, 128), 0)
    row = lax.broadcasted_iota(jnp.int32, (128, lanes), 0)

    def build_bias(b, carried):
        for half in range(2):
            value = rows_ref[b, half : half + 1, :] * LOG2E
            parts = jnp.zeros((128, HALF), jnp.float32)
            for n in range(3):
                part = value.astype(jnp.bfloat16).astype(jnp.float32)
                parts = jnp.where(row[:, 0:HALF] == n, part, parts)
                value = value - part
            bias_ref[b, half] = parts.T.astype(jnp.bfloat16)
        return carried

    lax.fori_loop(0, 32, build_bias, 0)

    for d in range(4):
        for n, dz in enumerate((1, -1)):
            index = at(z - dz, y - d, c)
            arrived(index)
            if d < 2 and dz == 1:
                sent.append(send(piece(index), at(z + 1, y, c), piece(index), s_up.at[4 + d], got.at[index]))
            if d >= 2 and dz == -1:
                sent.append(send(piece(index), at(z - 1, y, c), piece(index), s_down.at[2 + d], got.at[index]))
            sent.append(send(piece(index), at(z, y, 1 - c), piece(index), s_pair.at[4 + 2 * d + n], got.at[index]))
    for d in (0, 2, 1, 3):
        index = at(z + 2, y - d, c)
        arrived(index)
        sent.append(send(piece(index), at(z, y, 1 - c), piece(index), s_pair.at[12 + d], got.at[index]))

    def depart(d, carried):
        index = (me + d) % 32
        send(rows_out_ref.at[index], index, rows_in_ref.at[me], s_row.at[index], row_got.at[me])
        return carried

    lax.fori_loop(1, 32, depart, 0)
    mine = pltpu.make_async_copy(rows_out_ref.at[me], rows_in_ref.at[me], s_own.at[1])
    mine.start()

    for k in range(4):
        pltpu.make_async_copy(qt_ref.at[k], qt_ref.at[k], q_got.at[k]).wait()
    for zz in range(4):
        for yy in range(4):
            arrived(at(zz, yy, 1 - c))
    own.wait()

    def build(b, carried):
        pair = kv_all[b, 0:HALF, :].astype(jnp.float32)
        turned = pltpu.roll(pair, HEAD_DIM, axis=1)
        kk_ref[b, 0] = jnp.where(low_lane, pair, turned).astype(jnp.bfloat16)
        kk_ref[b, 1] = jnp.where(low_lane, turned, pair).astype(jnp.bfloat16)
        return carried

    lax.fori_loop(0, 32, build, 0)

    def later(x, n):
        return jnp.where(sub < RUNS - n, pltpu.roll(x, RUNS - n, axis=0), 1.0)

    def scores(b, half, z_ref):
        keys = jnp.concatenate([kk_ref[b, half], bias_ref[b, half]], axis=1)
        z_ref[...] = jnp.dot(keys, rhs_ref[...], preferred_element_type=jnp.float32)

    def weigh(z_ref, w_ref, first_key):
        for lane in range(0, lanes, 128):
            ls = slice(lane, lane + 128)
            us = []
            for i in range(RUN):
                u = jnp.exp2(jnp.minimum(z_ref[RUNS * i : RUNS * i + RUNS, ls], U_CAP))
                if first_key is not None:
                    query = lax.broadcasted_iota(jnp.int32, (RUNS, 128), 1) + lane
                    u = jnp.where(sub * RUN + (i + first_key) < query, u, 0.0)
                us.append(u)
            pairs = range(RUN // 2)
            rs = [1.0 / ((1.0 + us[2 * g]) * (1.0 + us[2 * g + 1])) for g in pairs]
            tree = list(rs)
            while len(tree) > 1:
                tree = [tree[2 * n] * tree[2 * n + 1] for n in range(len(tree) // 2)]
            total = tree[0]
            after = later(total, 1)
            after = after * later(after, 1)
            after = after * later(after, 2)
            after = after * later(after, 4)
            carry = carry_ref[:, ls]
            left = carry * after
            carry_ref[:, ls] = carry * jnp.broadcast_to((after * total)[0:1, :], (RUNS, 128))
            for g in reversed(pairs):
                left = left * rs[g]
                first = us[2 * g] * left
                second = us[2 * g + 1] * (left * (1.0 + us[2 * g]))
                both = jnp.concatenate([first, second], axis=0)
                w_ref[2 * RUNS * g : 2 * RUNS * g + 2 * RUNS, ls] = both.astype(jnp.bfloat16)

    def collect(b, half, w_ref):
        first = HALF + 2 * HEAD_DIM * half
        values = jnp.concatenate(
            [kv_all[b, first : first + HEAD_DIM, :], kv_all[b, first + HEAD_DIM : first + 2 * HEAD_DIM, :]], axis=1
        )
        acc_ref[...] += jnp.dot(values, w_ref[...], preferred_element_type=jnp.float32)

    def tile(n, carried):
        p = block_of(n, turn)
        scaled = qt_ref[n].astype(jnp.float32) * (LOG2E * HEAD_DIM**-0.5)
        top = scaled.astype(jnp.bfloat16)
        rhs_ref[0:HEAD_DIM, :] = top
        rhs_ref[HEAD_DIM : 2 * HEAD_DIM, :] = (scaled - top.astype(jnp.float32)).astype(jnp.bfloat16)
        rhs_ref[128:256, :] = jnp.where(row < 3, 1.0, 0.0).astype(jnp.bfloat16)
        carry_ref[...] = jnp.ones_like(carry_ref)
        acc_ref[...] = jnp.zeros_like(acc_ref)
        scores(p, 1, z_hi)
        scores(p, 0, z_lo)
        weigh(z_hi, w_hi, HALF)
        scores(jnp.maximum(p - 1, 0), 1, z_hi)
        weigh(z_lo, w_lo, 0)
        collect(p, 1, w_hi)

        def visit(step, inner):
            b = p - 1 - step
            scores(b, 0, z_lo)
            weigh(z_hi, w_hi, None)
            collect(b + 1, 0, w_lo)
            scores(jnp.maximum(b - 1, 0), 1, z_hi)
            weigh(z_lo, w_lo, None)
            collect(b, 1, w_hi)
            return inner

        lax.fori_loop(0, p, visit, 0)
        collect(0, 0, w_lo)
        done_ref[n] = acc_ref[...].astype(jnp.bfloat16)
        return carried

    lax.fori_loop(0, 4, tile, 0)

    for n in range(4):
        @pl.when(block_of(n, turn) != me)
        def _():
            send(done_ref.at[n], block_of(n, turn), home_ref.at[y], s_home.at[n], home_got.at[y])

        @pl.when(block_of(n, turn) == me)
        def _():
            pltpu.make_async_copy(done_ref.at[n], home_ref.at[y], home_got.at[y]).start()
    for h in range(4):
        pltpu.make_async_copy(home_ref.at[h], home_ref.at[h], home_got.at[h]).wait()

    def land(d, carried):
        index = (me + d) % 32
        pltpu.make_async_copy(rows_in_ref.at[index], rows_in_ref.at[index], row_got.at[index]).wait()
        pltpu.make_async_copy(rows_out_ref.at[index], rows_out_ref.at[index], s_row.at[index]).wait()
        return carried

    lax.fori_loop(1, 32, land, 0)
    mine.wait()
    for copy in sent:
        copy.wait_send()
    for h in range(4):
        @pl.when(q_dest(h) != me)
        def _():
            pltpu.make_async_copy(q_ref.at[h], q_ref.at[h], s_q.at[h]).wait()

        @pl.when(block_of(h, turn) != me)
        def _():
            pltpu.make_async_copy(done_ref.at[h], done_ref.at[h], s_home.at[h]).wait()


def mix(kv, q, bias, rows):
    whole = pl.BlockSpec(memory_space=pltpu.VMEM)
    anywhere = pl.BlockSpec(memory_space=pl.ANY)
    dma = pltpu.SemaphoreType.DMA
    bf16, f32 = jnp.bfloat16, jnp.float32
    return pl.pallas_call(
        mix_kernel,
        out_shape=(jax.ShapeDtypeStruct(q.shape, bf16), jax.ShapeDtypeStruct(rows.shape, bf16)),
        in_specs=[whole, whole, whole, anywhere],
        out_specs=(whole, anywhere),
        scratch_shapes=[
            pltpu.VMEM((32,) + kv.shape[1:], bf16),
            pltpu.VMEM(q.shape, bf16),
            pltpu.VMEM(q.shape, bf16),
            pltpu.VMEM((32, 2, HALF, 128), bf16),
            pltpu.VMEM((32, 2, HALF, 128), bf16),
            pltpu.VMEM((HALF, BLOCK), bf16),
            pltpu.VMEM((HALF, BLOCK), f32),
            pltpu.VMEM((HALF, BLOCK), f32),
            pltpu.VMEM((HALF, BLOCK), bf16),
            pltpu.VMEM((HALF, BLOCK), bf16),
            pltpu.VMEM((HEAD_DIM, BLOCK), f32),
            pltpu.VMEM((RUNS, BLOCK), f32),
            dma((32,)), dma((4,)), dma((4,)), dma((32,)),
            dma((3,)), dma((6,)), dma((6,)), dma((16,)), dma((4,)), dma((4,)), dma((32,)), dma((2,)),
        ],
        compiler_params=pltpu.CompilerParams(collective_id=1, has_side_effects=True),
        cost_estimate=pl.CostEstimate(flops=60_000_000_000, bytes_accessed=12 << 20, transcendentals=0),
        name="mix",
    )(kv, q, bias, rows)


def key_order(rows):
    n = rows.shape[-1]
    return rows.reshape(2, RUNS, RUN, n).swapaxes(1, 2).reshape(BLOCK, n)


def route(expert_pick, expert_total, capacity):
    picks = expert_pick.reshape(-1)
    matches = (picks[:, None] == jnp.arange(expert_total, dtype=jnp.int32)[None, :]).astype(jnp.int32)
    ranks = jnp.sum((jnp.cumsum(matches, axis=0) - matches) * matches, axis=1)
    return picks * capacity + ranks


def dot(a, b):
    return jnp.dot(a, b, preferred_element_type=jnp.float32)


def local(
    query_rows, key_rows, value_rows, key_bias, out_weight, moe_input, moe_gain,
    expert_pick, route_weight, w_gate, w_up, w_down,
):
    ep_index = lax.axis_index("ep")
    ep_count = lax.axis_size("ep")
    head = (ep_index >> 1) & 3
    token_count, width = moe_input.shape
    capacity = GROUPS * token_count // ep_count

    gates = lax.all_gather(w_gate[0], "tp")
    ups = lax.all_gather(w_up[0], "tp")
    downs = lax.all_gather(w_down[0], "tp", axis=0, tiled=True)

    q_heads = query_rows.T.reshape(4, HEAD_DIM, BLOCK)
    keys = key_order(key_rows).reshape(2, HALF, 4, HEAD_DIM)
    k_heads = keys.transpose(2, 1, 0, 3).reshape(4, HALF, 128)
    values = key_order(value_rows).T.reshape(4, HEAD_DIM, 4, 128)
    v_heads = values.transpose(0, 2, 1, 3).reshape(4, HALF, 128)
    kv = jnp.concatenate([k_heads, v_heads], axis=1)
    column = lax.dynamic_slice_in_dim(key_bias, head, 1, 1)
    bias = column.reshape(32, 2, RUNS, RUN).swapaxes(2, 3).reshape(32, 2, HALF)

    widened = moe_input.astype(jnp.float32)
    normed = (
        widened * lax.rsqrt(jnp.mean(widened * widened, axis=1, keepdims=True) + norm_eps) * moe_gain
    ).astype(jnp.bfloat16)
    slots = route(expert_pick, ep_count, capacity)
    owners = jnp.arange(slots.shape[0], dtype=jnp.int32) // TOPK
    table = jnp.full((ep_count * capacity,), token_count, jnp.int32).at[slots].set(owners)
    padded = jnp.concatenate([normed, jnp.zeros((1, width), jnp.bfloat16)], axis=0)
    outgoing = padded[table].reshape(ep_count, capacity, width)

    home, arrived = mix(kv, q_heads, bias, outgoing)

    part = jnp.einsum("cr,cm->rm", home.reshape(4 * HEAD_DIM, BLOCK), out_weight, preferred_element_type=jnp.float32)
    pieces = part.astype(jnp.bfloat16).reshape(4, 128, width)
    summed = lax.all_to_all(pieces, "tp", split_axis=0, concat_axis=0, tiled=True)
    mixer_out = summed.astype(jnp.float32).sum(axis=0).astype(jnp.bfloat16)

    rows = arrived.reshape(ep_count * capacity, width)
    gate_in = jnp.einsum("tm,smf->tsf", rows, gates, preferred_element_type=jnp.float32)
    up_in = jnp.einsum("tm,smf->tsf", rows, ups, preferred_element_type=jnp.float32)
    hidden = (jax.nn.silu(gate_in) * up_in).astype(jnp.bfloat16).reshape(rows.shape[0], -1)
    served = dot(hidden, downs).astype(jnp.bfloat16).reshape(ep_count, capacity, width)
    returned = lax.all_to_all(served, "ep", split_axis=0, concat_axis=0, tiled=True)
    flat = returned.reshape(ep_count * capacity, width)
    chosen = flat[slots].reshape(token_count, TOPK, width).astype(jnp.float32)
    routed_out = jnp.sum(chosen * route_weight[:, :, None], axis=1).astype(jnp.bfloat16)
    return (mixer_out, routed_out)


def solution(mesh):
    placed = (
        P("ep", "tp"), P("ep", "tp"), P("ep", "tp"), P(None, "tp"), P("tp", None),
        P(("ep", "tp"), None), P(), P(("ep", "tp"), None), P(("ep", "tp"), None),
        P("ep", None, "tp"), P("ep", None, "tp"), P("ep", "tp", None),
    )
    return jax.shard_map(
        local,
        mesh=mesh,
        in_specs=placed,
        out_specs=(P(("ep", "tp"), None), P(("ep", "tp"), None)),
        check_vma=False,
    )
```
